32 devices in a mesh: sp: 4 (over y, x), tp: 8 (over z, core).
Axes of the slice: x: 2, y: 2, z: 4, core: 2. Of those that a mesh axis runs over, the one named last changes fastest.
Arguments:
- residual_in: bfloat16 [2048, 4096], P('sp', 'tp'), may hold values from -24 to 24
- norm_gain: float32 [2, 4096], replicated, may hold values from 0.1 to 1.9
- gate_proj: bfloat16 [2, 4096, 2048], P(None, 'sp', 'tp'), may hold values from -0.09375 to 0.09375
- filter_proj: bfloat16 [2, 4096, 2048], P(None, 'sp', 'tp'), may hold values from -0.09375 to 0.09375
- signal_proj: bfloat16 [2, 4096, 2048], P(None, 'sp', 'tp'), may hold values from -0.09375 to 0.09375
- conv_taps: float32 [2, 3, 2048], P(None, None, 'tp'), may hold values from -3 to 3
- out_proj: bfloat16 [2, 2048, 4096], P(None, 'tp', 'sp'), may hold values from -0.1875 to 0.1875
- final_gain: float32 [4096], P('tp'), may hold values from 0.1 to 1.9
Outputs:
- final_rows: float32 [2048, 4096], P('sp', 'tp')
The draws below stay inside these ranges and needn't reach their ends.
All inputs are finite; a program needn't handle non-finite values.
Results may differ from the reference program's by a relative error of at most 0.033.
Values may be sent and summed in bfloat16 or wider, within the bound.
No kernel may reach another device: no remote copies, remote signals or barrier semaphores. Data moves between devices by JAX's collectives and lax.ppermute only.
A program may use at most 64 MiB of HBM per device.

```python
import math
import jax
import jax.numpy as jnp
from jax import lax

D = 4096
CW = 2048
TAPS = 3
LAYERS = 2
TOKENS = 2048
N_TP = 8


def draw_residual_in(key, part):
    subkeys = jax.random.split(key, 4)
    standard = jax.random.normal(subkeys[0], (TOKENS, D), jnp.float32)
    group_scale = jnp.exp(jax.random.uniform(subkeys[1], (D // 64,), jnp.float32, math.log(0.3), math.log(3.0)))
    column_scale = jnp.repeat(group_scale, 64)
    values = standard * column_scale[None, :]
    return jnp.clip(values, -24.0, 24.0).astype(jnp.bfloat16)


def spiked(values, rng, source, target, shards_of, factor):
    def block_of(position):
        return (jnp.arange(values.shape[position]) // (values.shape[position] // shards_of)).reshape((-1,) + (1,) * (values.ndim - 1 - position))

    near = jax.random.permutation(rng, shards_of)[block_of(target)]
    other_side = (block_of(target) + shards_of // 2) % shards_of
    return jnp.where((block_of(source) == near) | (block_of(source) == other_side), factor * values, values)


def block_levels(key, shape, pieces, least, high):
    def one(dim, blocks):
        heights = jax.random.uniform(jax.random.fold_in(jax.random.fold_in(key, 6), dim), (blocks,), jnp.float32, least / len(pieces), high / len(pieces))
        return jnp.repeat(jnp.exp(heights), shape[dim] // blocks).reshape((-1,) + (1,) * (len(shape) - dim - 1))

    loudness = one(*pieces[0])
    for cut in pieces[1:]:
        loudness = loudness * one(*cut)
    return loudness


def normal_values(own_key, dims, spread, most, cuts=(), held_as=jnp.bfloat16):
    result = jax.random.normal(own_key, dims, jnp.float32) * spread
    if len(cuts) > 0:
        result = block_levels(own_key, dims, cuts, -0.22, 0.18) * result
    return jnp.clip(result, min=-most, max=most).astype(held_as)


def heavy_noise(own_key, extent, scale, reach, shards, heavy, dtype=jnp.bfloat16):
    array = scale * jax.random.normal(own_key, extent, jnp.float32)
    if shards:
        array = array * block_levels(own_key, extent, shards, -0.22, 0.18)
    return jnp.clip(spiked(array, jax.random.fold_in(own_key, 3), *heavy), -reach, reach).astype(dtype)


def setup_inputs(seed: int = 0) -> dict:
    seeds = jax.random.split(jax.random.key(seed), 9)
    return {
        "residual_in": draw_residual_in(jax.random.fold_in(seeds[8], 71), 0),
        "norm_gain": jnp.clip(1.0 + 0.18 * jax.random.normal(seeds[1], (LAYERS, D), jnp.float32), 0.1, 1.9),
        "gate_proj": normal_values(seeds[2], (LAYERS, D, CW), D ** -0.5, 0.09375, ((1, 4), (2, 8))),
        "filter_proj": normal_values(seeds[3], (LAYERS, D, CW), D ** -0.5, 0.09375, ((1, 4), (2, 8))),
        "signal_proj": normal_values(seeds[4], (LAYERS, D, CW), D ** -0.5, 0.09375, ((1, 4), (2, 8))),
        "conv_taps": normal_values(seeds[5], (LAYERS, TAPS, CW), 0.6, 3.0, ((2, 8),), jnp.float32),
        "out_proj": heavy_noise(seeds[6], (LAYERS, CW, D), CW ** -0.5, 0.1875, ((1, 8), (2, 4)), (1, 2, 8, 2.0)),
        "final_gain": jnp.clip(1.0 + 0.18 * jax.random.normal(seeds[7], (D,), jnp.float32), 0.1, 1.9),
    }


norm_floor = 1e-06

def rms_scaled(values, gain_row):
    mean_square = lax.optimization_barrier(jnp.mean(values * values, axis=-1, keepdims=True))
    return values * lax.rsqrt(mean_square + norm_floor) * gain_row

def stored(values):
    return lax.optimization_barrier(values.astype(jnp.bfloat16)).astype(jnp.float32)

def causal_filter(product, taps):
    width_taps = taps.shape[0]
    length = product.shape[0]
    padded = jnp.concatenate([jnp.zeros((width_taps - 1, product.shape[1]), jnp.bfloat16), product], axis=0)
    filtered = jnp.zeros(product.shape, jnp.float32)
    for tap_index in range(width_taps):
        filtered = filtered + taps[tap_index] * padded[tap_index:tap_index + length].astype(jnp.float32)
    return filtered

def reference(residual_in, norm_gain, gate_proj, filter_proj, signal_proj, conv_taps, out_proj, final_gain):
    stream = residual_in
    block_width = CW // N_TP
    for layer_number in range(LAYERS):
        normed = rms_scaled(stream.astype(jnp.float32), norm_gain[layer_number]).astype(jnp.bfloat16)
        gate_rows = stored(jnp.dot(normed, gate_proj[layer_number], preferred_element_type=jnp.float32))
        filter_in = stored(jnp.dot(normed, filter_proj[layer_number], preferred_element_type=jnp.float32))
        signal_rows = stored(jnp.dot(normed, signal_proj[layer_number], preferred_element_type=jnp.float32))
        product = (filter_in * signal_rows).astype(jnp.bfloat16)
        filtered = causal_filter(product, conv_taps[layer_number])
        mixed_rows = (gate_rows * filtered).astype(jnp.bfloat16)
        branch = jnp.zeros((mixed_rows.shape[0], D), jnp.float32)
        for block_number in range(N_TP):
            lower_col = block_number * block_width
            partial_sum = jnp.dot(mixed_rows[:, lower_col:lower_col + block_width], out_proj[layer_number, lower_col:lower_col + block_width], preferred_element_type=jnp.float32)
            branch = branch + stored(partial_sum)
        stream = (stream.astype(jnp.float32) + branch).astype(jnp.bfloat16)
    return rms_scaled(stream.astype(jnp.float32), final_gain)
```

```python
import jax
import jax.numpy as jnp
from jax import lax
from jax.sharding import PartitionSpec as P

norm_floor = 1e-06
HALO = 8


def rounded(values):
    return values.astype(jnp.bfloat16)


def wide(values):
    return values.astype(jnp.float32)


def matmul(left, right):
    return jnp.dot(left, right, preferred_element_type=jnp.float32)


def causal(product, taps):
    rows = product.shape[0]
    padded = jnp.concatenate([jnp.zeros((taps.shape[0] - 1, product.shape[1]), product.dtype), product], axis=0)
    filtered = jnp.zeros(product.shape, jnp.float32)
    for k in range(taps.shape[0]):
        filtered = filtered + taps[k] * wide(padded[k : k + rows])
    return filtered


def make(mesh):
    n_sp, n_tp = mesh.shape["sp"], mesh.shape["tp"]
    n_z = n_tp // 2

    def sp_xor(value, mask):
        return lax.ppermute(value, "sp", [(i, i ^ mask) for i in range(n_sp)])

    def z_move(value, pairs):
        return lax.ppermute(value, "tp", [(2 * a + c, 2 * b + c) for a, b in pairs for c in range(2)])

    def core_swap(value):
        return lax.ppermute(value, "tp", [(i, i ^ 1) for i in range(n_tp)])

    def gathered(own):
        beside = sp_xor(own, 1)
        across = sp_xor(own, 2)
        half = own.shape[0] // 2
        first = sp_xor(across[:half], 1)
        second = sp_xor(beside[half:], 2)
        return [own, beside, across, jnp.concatenate([first, second], axis=0)]

    def per_device(residual_in, norm_gain, gate_proj, filter_proj, signal_proj, conv_taps, out_proj, final_gain):
        layers = norm_gain.shape[0]
        width = norm_gain.shape[1]
        tokens, piece = residual_in.shape
        rows = tokens + HALO
        channels = gate_proj.shape[2]
        s = lax.axis_index("sp")
        t = lax.axis_index("tp")
        z, c = t // 2, t % 2

        halo = lax.ppermute(residual_in[tokens - HALO :], "sp", [(i, i + 1) for i in range(n_sp - 1)])
        own = jnp.concatenate([halo, residual_in], axis=0)

        w_in = [jnp.concatenate([filter_proj[l], signal_proj[l], gate_proj[l]], axis=1) for l in range(layers)]
        in_shards = [None] * layers
        out_shards = [None] * layers
        for l in range(layers):
            in_shards[l] = gathered(w_in[l])
            out_shards[l] = gathered(out_proj[l])

        up, down = own, own
        from_low, from_high = [None] * n_z, [None] * n_z
        for k in range(1, n_z):
            up = z_move(up, [(i, i + 1) for i in range(k - 1, n_z - 1)])
            down = z_move(down, [(i, i - 1) for i in range(n_z - k, 0, -1)])
            from_low[k], from_high[k] = up, down
        mine = jnp.stack(
            [own] + [jnp.where(z >= k, from_low[k], from_high[n_z - k]) for k in range(1, n_z)], axis=0
        )
        theirs = core_swap(mine)

        def at_block(stack, index):
            return lax.dynamic_index_in_dim(stack, index, 0, keepdims=False)

        x_mine, x_theirs = [], []
        for j in range(n_sp):
            index = (z - (s ^ j)) % n_z
            x_mine.append(at_block(mine, index))
            x_theirs.append(at_block(theirs, index))

        for l in range(layers):
            square_sum = jnp.zeros((rows, 1), jnp.float32)
            total = jnp.zeros((rows, 3 * channels), jnp.float32)
            for j in range(n_sp):
                base = (s ^ j) * (2 * piece)
                for value, core in ((x_mine[j], c), (x_theirs[j], 1 - c)):
                    value = wide(value)
                    square_sum = square_sum + jnp.sum(value * value, axis=1, keepdims=True)
                    gain = lax.dynamic_slice(norm_gain[l], (base + core * piece,), (piece,))
                    block = lax.dynamic_slice(in_shards[l][j], (core * piece, 0), (piece, 3 * channels))
                    total = total + matmul(rounded(value * gain), block)
            total = rounded(total * lax.rsqrt(square_sum / width + norm_floor))
            total = lax.optimization_barrier(total)
            product = rounded(wide(total[:, :channels]) * wide(total[:, channels : 2 * channels]))
            mixed = rounded(wide(total[:, 2 * channels :]) * causal(product, conv_taps[l]))
            parts = []
            for j in range(n_sp):
                part = rounded(matmul(mixed, out_shards[l][j]))
                keep = lax.dynamic_slice(part, (0, c * piece), (rows, piece))
                give = lax.dynamic_slice(part, (0, (1 - c) * piece), (rows, piece))
                parts.append((keep, give))
            if l < layers - 1:
                new_mine, new_theirs = [], []
                for j in range(n_sp):
                    keep, give = parts[j]
                    acc = rounded(wide(keep) + wide(core_swap(give)))
                    for hop in range(n_z // 2 - 1):
                        got = z_move(acc, [(hop, hop + 1), (n_z - 1 - hop, n_z - 2 - hop)])
                        acc = rounded(wide(acc) + wide(got))
                    mid = n_z // 2
                    got = z_move(acc, [(mid - 1, mid), (mid, mid - 1)])
                    block = rounded(wide(x_mine[j]) + (wide(acc) + wide(got)))
                    for hop in range(n_z // 2 - 2, -1, -1):
                        got = z_move(block, [(hop + 1, hop), (n_z - 2 - hop, n_z - 1 - hop)])
                        block = jnp.where((z <= hop) | (z >= n_z - 1 - hop), got, block)
                    new_mine.append(block)
                    new_theirs.append(core_swap(block))
                x_mine, x_theirs = new_mine, new_theirs

        stack = jnp.stack(
            [rounded(wide(keep[HALO:]) + wide(core_swap(give[HALO:]))) for keep, give in parts], axis=0
        )
        up = jnp.zeros((tokens, piece), jnp.float32)
        down = up
        last = n_z - 1
        for k in range(last):
            send_up = rounded(wide(at_block(stack, s ^ jnp.minimum(z + last - k, last))) + up)
            send_down = rounded(wide(at_block(stack, s ^ jnp.maximum(z - last + k, 0))) + down)
            up = wide(z_move(send_up, [(i, i + 1) for i in range(k + 1)]))
            down = wide(z_move(send_down, [(i, i - 1) for i in range(last, last - k - 1, -1)]))
        stream = at_block(jnp.stack(x_mine, axis=0), s ^ z)[HALO:]
        branch = wide(at_block(stack, s ^ z)) + (up + down)
        stream = wide(rounded(wide(stream) + branch))
        square_sum = lax.psum(jnp.sum(stream * stream, axis=1, keepdims=True), "tp")
        return stream * lax.rsqrt(square_sum / width + norm_floor) * final_gain

    def plain(residual_in, norm_gain, gate_proj, filter_proj, signal_proj, conv_taps, out_proj, final_gain):
        layers, width = norm_gain.shape
        keep = conv_taps.shape[1] - 1
        whole_in = [lax.all_gather(w, "sp", axis=1, tiled=True) for w in (filter_proj, signal_proj, gate_proj)]
        whole_out = lax.all_gather(out_proj, "sp", axis=2, tiled=True)
        stream = residual_in
        for l in range(layers):
            full = wide(lax.all_gather(stream, "tp", axis=1, tiled=True))
            mean_square = jnp.mean(full * full, axis=-1, keepdims=True)
            normed = rounded(full * lax.rsqrt(mean_square + norm_floor) * norm_gain[l])
            filter_in, signal, gate = [rounded(matmul(normed, w[l])) for w in whole_in]
            product = rounded(wide(filter_in) * wide(signal))
            edge = lax.ppermute(product[product.shape[0] - keep :], "sp", [(i, i + 1) for i in range(n_sp - 1)])
            filtered = causal(jnp.concatenate([edge, product], axis=0), conv_taps[l])[keep:]
            mixed = rounded(wide(gate) * filtered)
            part = rounded(matmul(mixed, whole_out[l]))
            branch = wide(lax.psum_scatter(part, "tp", scatter_dimension=1, tiled=True))
            stream = rounded(wide(stream) + branch)
        stream = wide(stream)
        square_sum = lax.psum(jnp.sum(stream * stream, axis=1, keepdims=True), "tp")
        return stream * lax.rsqrt(square_sum / width + norm_floor) * final_gain

    return per_device if n_sp == n_z and n_sp == 4 else plain


def solution(mesh):
    return jax.shard_map(
        make(mesh),
        mesh=mesh,
        in_specs=(
            P("sp", "tp"),
            P(),
            P(None, "sp", "tp"),
            P(None, "sp", "tp"),
            P(None, "sp", "tp"),
            P(None, None, "tp"),
            P(None, "tp", "sp"),
            P("tp"),
        ),
        out_specs=P("sp", "tp"),
        check_vma=False,
    )
```
